32 devices in a mesh: ep: 8 (over z, x), tp: 4 (over y, core).
Axes of the slice: x: 2, y: 2, z: 4, core: 2. Of those that a mesh axis runs over, the one named last changes fastest.
Arguments:
- tokens: bfloat16 [128, 2048], P('ep'), may hold values from -6 to 6
- norm_attn: float32 [2048], replicated, may hold values from 0.1 to 1.9
- w_query: bfloat16 [2048, 1024], P(None, 'tp'), may hold values from -0.125 to 0.125
- w_key: bfloat16 [2048, 1024], P(None, 'tp'), may hold values from -0.125 to 0.125
- w_value: bfloat16 [2048, 1024], P(None, 'tp'), may hold values from -0.125 to 0.125
- w_forget: bfloat16 [2048, 16], P(None, 'tp'), may hold values from -0.125 to 0.125
- forget_bias: float32 [16], P('tp'), may hold values from -1.5 to 1.5
- w_output: bfloat16 [1024, 2048], P('tp'), may hold values from -0.1875 to 0.1875
- key_cache: bfloat16 [128, 1024, 1024], P('ep', None, 'tp'), may hold values from -488 to 488
- value_cache: bfloat16 [128, 1024, 1024], P('ep', None, 'tp'), may hold values from -6 to 6
- gate_cache: float32 [128, 16, 1024], P('ep', 'tp'), may hold values from -132 to 0, as said below
- lengths: int32 [128], P('ep'), may hold values from 256 to 1024
- norm_ffn: float32 [2048], replicated, may hold values from 0.1 to 1.9
- route_group: int32 [128], P('ep'), may hold values from 0 to 3
- route_slot: int32 [128, 2], P('ep'), may hold values from 0 to 7, as said below
- route_weight: float32 [128, 2], P('ep'), may hold values from 0.2 to 1
- expert_gate: bfloat16 [32, 2048, 1024], P('ep', None, 'tp'), may hold values from -0.125 to 0.125
- expert_up: bfloat16 [32, 2048, 1024], P('ep', None, 'tp'), may hold values from -0.125 to 0.125
- expert_down: bfloat16 [32, 1024, 2048], P('ep', 'tp'), may hold values from -0.1875 to 0.1875
- dense_gate: bfloat16 [2048, 4096], P('tp', 'ep'), may hold values from -0.125 to 0.125
- dense_up: bfloat16 [2048, 4096], P('tp', 'ep'), may hold values from -0.125 to 0.125
- dense_down: bfloat16 [4096, 2048], P('ep', 'tp'), may hold values from -0.09375 to 0.09375
- mix_vector: float32 [2048], replicated, may hold values from -0.125 to 0.125
Outputs:
- mixed_out: bfloat16 [128, 2048], P('ep', 'tp')
The draws below stay inside these ranges and needn't reach their ends.
Inputs may be any that keep to these rules, and one draw needn't show every extreme that they name: `route_slot`: the two picks of a token are different experts of its group. Among the sequences of one index of ep at most 2 picks name one expert, and in every draw some expert gets exactly 2 picks from every index of ep. `gate_cache`: along the positions of each sequence and head the values never rise.
All inputs are finite; a program needn't handle non-finite values.
Results may differ from the reference program's by a relative error of at most 0.014.
Values may be sent and summed in bfloat16 or wider, within the bound.
A program may use at most 128 MiB of HBM per device.

```python
import jax
import jax.numpy as jnp
import numpy as np
from jax import lax

D = 2048
HEADS = 16
HEAD_DIM = 64
GROUPS = 4
EXPERTS_PER_GROUP = 8
EXPERT_FF = 1024
DENSE_FF = 4096
TOP_K = 2
SEQ_DEV = 16
STORED_ENTRIES = 1024
EXPERTS = 32
STREAM_COUNT = 128
N_TP = 4


def routing_table(key):
    block_count = STREAM_COUNT // SEQ_DEV
    quarter = SEQ_DEV // 4
    eighth = SEQ_DEV // 8
    group_sizes = [SEQ_DEV // 2, quarter, eighth, SEQ_DEV - SEQ_DEV // 2 - quarter - eighth]
    member = np.concatenate([np.full(size_now, order_now) for order_now, size_now in enumerate(group_sizes)]).astype(np.int32)
    within = np.concatenate([np.arange(size_now) for size_now in group_sizes]).astype(np.int32)
    hot_order = jax.random.permutation(jax.random.fold_in(key, 11), GROUPS)

    def one_block(block_index):
        block_key = jax.random.fold_in(jax.random.fold_in(key, 12), block_index)
        derived_seeds = jax.random.split(block_key, 4)
        rest_order = jax.random.permutation(derived_seeds[0], GROUPS - 1)
        own_order = jnp.concatenate([hot_order[:1], hot_order[1:][rest_order]])
        is_hot = jax.random.randint(derived_seeds[1], (), 0, 2)
        group_order = jnp.where(is_hot == 1, hot_order, own_order)
        expert_orders = jax.vmap(lambda one_key: jax.random.permutation(one_key, EXPERTS_PER_GROUP))(jax.random.split(derived_seeds[2], GROUPS))
        groups = group_order[member]
        first_slot = expert_orders[member, within % EXPERTS_PER_GROUP]
        second = expert_orders[member, (within + 1) % EXPERTS_PER_GROUP]
        shuffle = jax.random.permutation(derived_seeds[3], SEQ_DEV)
        return (groups[shuffle], jnp.stack([first_slot, second], axis=1)[shuffle])
    groups, slots = jax.vmap(one_block)(jnp.arange(block_count))
    return (groups.reshape(-1).astype(jnp.int32), slots.reshape(-1, 2).astype(jnp.int32))


def draw_route_group(key, part):
    return routing_table(jax.random.fold_in(key, 5))[0]


def draw_route_slot(key, part):
    return routing_table(jax.random.fold_in(key, 5))[1]


def draw_gate_cache(key, part):
    derived_seeds = jax.random.split(key, 5)
    lagging_marker = jax.random.randint(derived_seeds[0], (HEADS,), 0, 2).astype(jnp.float32)
    step_rate = lagging_marker * (1.0 / STORED_ENTRIES) + (1.0 - lagging_marker) * (1.0 / 40.0)
    seq_scale = jnp.exp(jax.random.uniform(derived_seeds[1], (STREAM_COUNT, 1, 1), jnp.float32, -0.7, 0.7))
    roughness = jnp.exp(jax.random.uniform(derived_seeds[2], (STREAM_COUNT, HEADS, STORED_ENTRIES), jnp.float32, -0.7, 0.7))
    recorded_moments = -step_rate[None, :, None] * seq_scale * roughness
    run_opening = jax.random.randint(derived_seeds[3], (STREAM_COUNT, 3), 0, STORED_ENTRIES)
    entry_indices = jnp.arange(STORED_ENTRIES)
    run_extents = jnp.any(entry_indices[None, None, :] == run_opening[:, :, None], axis=1).astype(jnp.float32)
    run_extent = jnp.log(jax.random.uniform(derived_seeds[4], (STREAM_COUNT, 1, STORED_ENTRIES), jnp.float32, 0.5, 0.8))
    recorded_moments = recorded_moments + run_extents[:, None, :] * lagging_marker[None, :, None] * run_extent
    return jnp.cumsum(recorded_moments, axis=-1)


def draw_key_cache(key, part):
    derived_seeds = jax.random.split(key, 1)
    width_all = HEADS * HEAD_DIM
    base = jnp.clip(jax.random.normal(derived_seeds[0], (STREAM_COUNT, STORED_ENTRIES, width_all), jnp.float32), -4.0, 4.0)
    return base.astype(jnp.bfloat16)


def touch_ends(values, own_key, smallest, largest):
    longest = values.shape.index(max(values.shape))
    spots = []
    for shift in (0, 1):
        where = [jax.random.randint(jax.random.fold_in(own_key, axis), (), 0, length) for axis, length in enumerate(values.shape)]
        where[longest] = (where[longest] + shift) % values.shape[longest]
        spots.append(tuple(where))
    return values.at[spots[0]].set(smallest).at[spots[1]].set(largest)


def level_of(key, shape, cuts, least, top_value):
    def one(axis_at, shards_of):
        steps = jax.random.uniform(jax.random.fold_in(jax.random.fold_in(key, 6), axis_at), (shards_of,), jnp.float32, least / len(cuts), top_value / len(cuts))
        return jnp.repeat(jnp.exp(steps), shape[axis_at] // shards_of).reshape((-1,) + (1,) * (len(shape) - axis_at - 1))

    gain = one(*cuts[0])
    for cut in cuts[1:]:
        gain = gain * one(*cut)
    return gain


def centred(stream_key, extent, scale, reach, cuts=(), held_as=jnp.bfloat16):
    entries = jax.random.normal(stream_key, extent, jnp.float32) * scale
    if len(cuts) > 0:
        entries = level_of(stream_key, extent, cuts, -0.22, 0.18) * entries
    return jnp.clip(entries, min=-reach, max=reach).astype(held_as)


def setup_inputs(seed: int = 0) -> dict:
    splits = jax.random.split(jax.random.key(seed), 24)
    return {
        "tokens": centred(splits[0], (STREAM_COUNT, D), 1.0, 6.0, ((0, 8),)),
        "norm_attn": jnp.clip(1.0 + 0.18 * jax.random.normal(splits[1], (D,), jnp.float32), 0.1, 1.9),
        "w_query": centred(splits[2], (D, HEADS * HEAD_DIM), D ** -0.5, 0.125, ((1, 4),)),
        "w_key": centred(splits[3], (D, HEADS * HEAD_DIM), D ** -0.5, 0.125, ((1, 4),)),
        "w_value": centred(splits[4], (D, HEADS * HEAD_DIM), D ** -0.5, 0.125, ((1, 4),)),
        "w_forget": centred(splits[5], (D, HEADS), D ** -0.5, 0.125, ((1, 4),)),
        "forget_bias": jnp.clip(jax.random.uniform(splits[6], (HEADS,), jnp.float32, -1.5, 1.5) * level_of(splits[6], (HEADS,), ((0, 4),), -0.4, 0.0), -1.5, 1.5),
        "w_output": centred(splits[7], (HEADS * HEAD_DIM, D), (HEADS * HEAD_DIM) ** -0.5, 0.1875, ((0, 4),)),
        "key_cache": draw_key_cache(jax.random.fold_in(splits[23], 71), 0),
        "value_cache": centred(splits[9], (STREAM_COUNT, STORED_ENTRIES, HEADS * HEAD_DIM), 1.0, 6.0, ((0, 8), (2, 4))),
        "gate_cache": draw_gate_cache(jax.random.fold_in(splits[23], 71), 0),
        "lengths": touch_ends(jax.random.randint(splits[11], (STREAM_COUNT,), STORED_ENTRIES // 4, STORED_ENTRIES + 1), jax.random.fold_in(splits[11], 1), STORED_ENTRIES // 4, STORED_ENTRIES).astype(jnp.int32),
        "norm_ffn": jnp.clip(1.0 + 0.18 * jax.random.normal(splits[12], (D,), jnp.float32), 0.1, 1.9),
        "route_group": draw_route_group(jax.random.fold_in(splits[23], 71), 0),
        "route_slot": draw_route_slot(jax.random.fold_in(splits[23], 71), 0),
        "route_weight": jnp.clip(0.2 + 0.8 * jax.random.uniform(splits[15], (STREAM_COUNT, TOP_K), jnp.float32) ** level_of(splits[15], (STREAM_COUNT, TOP_K), ((0, 8),), -0.2, 0.2), 0.2, 1.0),
        "expert_gate": centred(splits[16], (EXPERTS, D, EXPERT_FF), D ** -0.5, 0.125, ((0, 8), (2, 4))),
        "expert_up": centred(splits[17], (EXPERTS, D, EXPERT_FF), D ** -0.5, 0.125, ((0, 8), (2, 4))),
        "expert_down": centred(splits[18], (EXPERTS, EXPERT_FF, D), EXPERT_FF ** -0.5, 0.1875, ((0, 8), (1, 4))),
        "dense_gate": centred(splits[19], (D, DENSE_FF), D ** -0.5, 0.125, ((0, 4), (1, 8))),
        "dense_up": centred(splits[20], (D, DENSE_FF), D ** -0.5, 0.125, ((0, 4), (1, 8))),
        "dense_down": centred(splits[21], (DENSE_FF, D), DENSE_FF ** -0.5, 0.09375, ((0, 8), (1, 4))),
        "mix_vector": centred(splits[22], (D,), D ** -0.5, 0.125, (), jnp.float32),
    }


EPS = 1e-06

def rms_scale(row_block, gain_vector):
    row_block = row_block.astype(jnp.float32)
    return row_block * lax.rsqrt(lax.optimization_barrier(jnp.mean(row_block * row_block, axis=-1, keepdims=True)) + EPS) * gain_vector

def bf16_round(array):
    return lax.optimization_barrier(array.astype(jnp.bfloat16)).astype(jnp.float32)

def attend_one(packed):
    queries, key_new, value_new, forget_log, key_rows, value_rows, gate_row, length = packed
    heads = gate_row.shape[0]
    cache_len = gate_row.shape[1]
    head_size = queries.shape[0] // heads
    score_scale = head_size ** (-0.5)
    query_h = queries.astype(jnp.float32).reshape(heads, head_size)
    key_h = key_rows.astype(jnp.float32).reshape(cache_len, heads, head_size)
    value_h = value_rows.astype(jnp.float32).reshape(cache_len, heads, head_size)
    entry_indices = jnp.arange(cache_len, dtype=jnp.int32)
    last_gate = lax.optimization_barrier(jnp.sum(jnp.where(entry_indices[None, :] == length - 1, gate_row, jnp.zeros_like(gate_row)), axis=1))
    current = last_gate + forget_log
    scores = jnp.einsum('hd,jhd->hj', query_h, key_h) * score_scale + (current[:, None] - gate_row)
    scores = jnp.where(entry_indices[None, :] < length, scores, -jnp.inf)
    own_score = lax.optimization_barrier(jnp.sum(query_h * key_new.astype(jnp.float32).reshape(heads, head_size), axis=1)) * score_scale
    row_peak = jnp.maximum(lax.optimization_barrier(jnp.max(scores, axis=1)), own_score)
    weights = jnp.exp(scores - row_peak[:, None])
    own_weight = jnp.exp(own_score - row_peak)
    denominator = lax.optimization_barrier(jnp.sum(weights, axis=1)) + own_weight
    weighted = jnp.einsum('hj,jhd->hd', bf16_round(weights), value_h)
    weighted = weighted + bf16_round(own_weight)[:, None] * value_new.astype(jnp.float32).reshape(heads, head_size)
    return (weighted / denominator[:, None]).astype(jnp.bfloat16).reshape(-1)

def reference(tokens, norm_attn, w_query, w_key, w_value, w_forget, forget_bias, w_output, key_cache, value_cache, gate_cache, lengths, norm_ffn, route_group, route_slot, route_weight, expert_gate, expert_up, expert_down, dense_gate, dense_up, dense_down, mix_vector):
    normed = rms_scale(tokens, norm_attn).astype(jnp.bfloat16)
    queries = jnp.dot(normed, w_query, preferred_element_type=jnp.float32).astype(jnp.bfloat16)
    key_new = jnp.dot(normed, w_key, preferred_element_type=jnp.float32).astype(jnp.bfloat16)
    value_new = jnp.dot(normed, w_value, preferred_element_type=jnp.float32).astype(jnp.bfloat16)
    forget_log = jax.nn.log_sigmoid(jnp.dot(normed, w_forget, preferred_element_type=jnp.float32) + forget_bias)
    attended = lax.map(attend_one, (queries, key_new, value_new, forget_log, key_cache, value_cache, gate_cache, lengths))
    head_block = HEADS * HEAD_DIM // N_TP
    head_parts = jnp.einsum('snr,nrd->snd', attended.astype(jnp.float32).reshape(STREAM_COUNT, N_TP, head_block), w_output.astype(jnp.float32).reshape(N_TP, head_block, D))
    attn_sum = lax.optimization_barrier(jnp.sum(bf16_round(head_parts), axis=1))
    residual = tokens.astype(jnp.float32) + attn_sum
    normed_ffn = rms_scale(residual, norm_ffn).astype(jnp.bfloat16)
    expert_ids = route_group[:, None] * EXPERTS_PER_GROUP + route_slot
    ff_block = EXPERT_FF // N_TP

    def expert_term(expert, running):
        coefficient = lax.optimization_barrier(jnp.sum(jnp.where(expert_ids == expert, route_weight, jnp.zeros_like(route_weight)), axis=1))
        gate_act = jnp.dot(normed_ffn, expert_gate[expert], preferred_element_type=jnp.float32)
        up_act = jnp.dot(normed_ffn, expert_up[expert], preferred_element_type=jnp.float32)
        hidden = (jax.nn.silu(gate_act) * up_act).astype(jnp.bfloat16)
        partial_value = jnp.einsum('snf,nfd->snd', hidden.astype(jnp.float32).reshape(STREAM_COUNT, N_TP, ff_block), expert_down[expert].astype(jnp.float32).reshape(N_TP, ff_block, D))
        result = bf16_round(lax.optimization_barrier(jnp.sum(bf16_round(partial_value), axis=1)))
        return running + coefficient[:, None] * result
    moe = lax.fori_loop(0, EXPERTS, expert_term, jnp.zeros((STREAM_COUNT, D), jnp.float32))
    feature_block = D // N_TP
    grouped = normed_ffn.astype(jnp.float32).reshape(STREAM_COUNT, N_TP, feature_block)
    gate_parts = jnp.einsum('snd,ndf->snf', grouped, dense_gate.astype(jnp.float32).reshape(N_TP, feature_block, DENSE_FF))
    up_parts = jnp.einsum('snd,ndf->snf', grouped, dense_up.astype(jnp.float32).reshape(N_TP, feature_block, DENSE_FF))
    gate_sum = lax.optimization_barrier(jnp.sum(bf16_round(gate_parts), axis=1))
    up_sum = lax.optimization_barrier(jnp.sum(bf16_round(up_parts), axis=1))
    dense_hidden = (jax.nn.silu(gate_sum) * up_sum).astype(jnp.bfloat16)
    dense_out = jnp.dot(dense_hidden, dense_down, preferred_element_type=jnp.float32)
    mix_gate = jax.nn.sigmoid(jnp.dot(normed_ffn.astype(jnp.float32), mix_vector, precision=lax.Precision.HIGHEST))
    return (residual + moe + mix_gate[:, None] * dense_out).astype(jnp.bfloat16)
```

```python
import functools

import jax
import jax.numpy as jnp
from jax import lax
from jax.experimental import pallas as pl
from jax.experimental.pallas import tpu as pltpu
from jax.sharding import PartitionSpec as P

EXPERTS_PER_GROUP = 8


EPS = 1e-06
F32 = jnp.float32
BF16 = jnp.bfloat16
MESH = pl.DeviceIdType.MESH
VMEM = pl.BlockSpec(memory_space=pltpu.VMEM)
NT = (((1,), (1,)), ((), ()))


def rms_scale(row_block, gain):
    return row_block * lax.rsqrt(jnp.mean(row_block * row_block, axis=-1, keepdims=True) + EPS) * gain


def attend_kernel(
    batch, len_ref, tok_ref, gain_ref, wq_ref, wk_ref, wv_ref, wf_ref, bias_ref, wo_ref,
    key_ref, value_ref, gate_ref, out_ref, q_scr, k_scr, v_scr, f_scr, a_scr,
):
    step = pl.program_id(0)
    heads = wf_ref.shape[0]
    width = wq_ref.shape[1]
    cache_len = key_ref.shape[1]
    head_size = width // heads
    score_scale = head_size ** (-0.5)

    @pl.when(step == 0)
    def _():
        normed = rms_scale(tok_ref[...].astype(F32), gain_ref[...]).astype(BF16)
        for w_ref, scr in ((wq_ref, q_scr), (wk_ref, k_scr), (wv_ref, v_scr)):
            made = jnp.dot(normed, w_ref[...], preferred_element_type=F32)
            scr[...] = made.astype(BF16).astype(F32)
        logit = lax.dot_general(wf_ref[...], normed, NT, preferred_element_type=F32)
        f_scr[...] = jax.nn.log_sigmoid(logit + bias_ref[...])

    head_of = lax.broadcasted_iota(jnp.int32, (heads, width), 1) // head_size
    mine = head_of == lax.broadcasted_iota(jnp.int32, (heads, width), 0)
    position = lax.broadcasted_iota(jnp.int32, (heads, cache_len), 1)
    seq_lane = lax.broadcasted_iota(jnp.int32, f_scr.shape, 1)
    for i in range(batch):
        s = step * batch + i
        length = len_ref[s]
        query = q_scr[pl.ds(s, 1), :]
        query_heads = jnp.where(mine, query, 0.0)
        gate = gate_ref[i]
        forget = jnp.sum(jnp.where(seq_lane == s, f_scr[...], 0.0), axis=1, keepdims=True)
        last = jnp.sum(jnp.where(position == length - 1, gate, 0.0), axis=1, keepdims=True)
        scores = lax.dot_general(
            query_heads.astype(BF16), key_ref[i], NT, preferred_element_type=F32
        ) * score_scale
        scores = scores + ((last + forget) - gate)
        scores = jnp.where(position < length, scores, -jnp.inf)
        own = jnp.sum(query_heads * k_scr[pl.ds(s, 1), :], axis=1, keepdims=True) * score_scale
        peak = jnp.maximum(jnp.max(scores, axis=1, keepdims=True), own)
        weights = jnp.exp(scores - peak)
        own_weight = jnp.exp(own - peak)
        denominator = jnp.sum(weights, axis=1, keepdims=True) + own_weight
        weighted = jnp.dot(weights.astype(BF16), value_ref[i], preferred_element_type=F32)
        weighted = weighted + own_weight.astype(BF16).astype(F32) * v_scr[pl.ds(s, 1), :]
        result = jnp.where(mine, weighted / denominator, 0.0)
        a_scr[pl.ds(s, 1), :] = jnp.sum(result, axis=0, keepdims=True)

    @pl.when(step == pl.num_programs(0) - 1)
    def _():
        out_ref[...] = jnp.dot(
            a_scr[...].astype(BF16), wo_ref[...], preferred_element_type=F32
        ).astype(BF16)


def attention(tokens, gain, wq, wk, wv, wf, bias, wo, key_cache, value_cache, gate_cache, lengths):
    seqs, model = tokens.shape
    _, cache_len, width = key_cache.shape
    heads = gate_cache.shape[1]
    batch = 4 if seqs % 4 == 0 else 1
    whole = lambda shape: pl.BlockSpec(shape, lambda i: (0,) * len(shape))
    return pl.pallas_call(
        functools.partial(attend_kernel, batch),
        grid=(seqs // batch,),
        out_shape=jax.ShapeDtypeStruct((seqs, model), BF16),
        in_specs=[
            pl.BlockSpec(memory_space=pltpu.SMEM),
            whole((seqs, model)),
            whole((1, model)),
            whole(wq.shape),
            whole(wk.shape),
            whole(wv.shape),
            whole((heads, model)),
            whole((heads, 1)),
            whole(wo.shape),
            pl.BlockSpec((batch, cache_len, width), lambda i: (i, 0, 0)),
            pl.BlockSpec((batch, cache_len, width), lambda i: (i, 0, 0)),
            pl.BlockSpec((batch, heads, cache_len), lambda i: (i, 0, 0)),
        ],
        out_specs=whole((seqs, model)),
        scratch_shapes=[
            pltpu.VMEM((seqs, width), F32),
            pltpu.VMEM((seqs, width), F32),
            pltpu.VMEM((seqs, width), F32),
            pltpu.VMEM((heads, seqs), F32),
            pltpu.VMEM((seqs, width), F32),
        ],
        compiler_params=pltpu.CompilerParams(
            dimension_semantics=("arbitrary",), vmem_limit_bytes=48 * 1024 * 1024
        ),
        name="attend",
    )(
        lengths, tokens, gain[None, :], wq, wk, wv, wf.T, bias[:, None], wo,
        key_cache, value_cache, gate_cache,
    )


def greet(axis, count):
    me = lax.axis_index(axis)
    barrier = pltpu.get_barrier_semaphore()
    for k in range(1, count):
        pl.semaphore_signal(
            barrier, inc=1, device_id={axis: lax.rem(me + k, count)}, device_id_type=MESH
        )
    pl.semaphore_wait(barrier, count - 1)
    return me


def remote(axis, peer, src, dst, send, recv):
    copy = pltpu.make_async_remote_copy(
        src_ref=src, dst_ref=dst, send_sem=send, recv_sem=recv,
        device_id={axis: peer}, device_id_type=MESH,
    )
    copy.start()
    return copy


def comm_params(number):
    return pltpu.CompilerParams(
        collective_id=number, has_side_effects=True, vmem_limit_bytes=32 * 1024 * 1024
    )


def residual_kernel(
    count, part_ref, tok_ref, gain_ref, table_ref, res_ref, norm_ref, out_ref, land, send, recv
):
    me = greet("tp", count)
    copies = [
        remote("tp", lax.rem(me + k, count), part_ref, land.at[k - 1], send.at[k - 1], recv.at[k - 1])
        for k in range(1, count)
    ]
    total = part_ref[...].astype(F32)
    for k in range(1, count):
        copies[k - 1].wait_recv()
        total = total + land[k - 1].astype(F32)
    residual = tok_ref[...].astype(F32) + total
    res_ref[...] = residual
    normed = rms_scale(residual, gain_ref[...]).astype(BF16)
    norm_ref[...] = normed
    out_ref[...] = jnp.dot(table_ref[...], normed, preferred_element_type=F32).astype(BF16)
    for copy in copies:
        copy.wait_send()


def spread_kernel(count, tp_count, rows_ref, norm_ref, arr_ref, por_ref, land_a, land_p, sems):
    me = greet("ep", count)
    width = por_ref.shape[2]
    own_cols = pl.ds(pl.multiple_of(lax.axis_index("tp") * width, width), width)
    copies = []
    for k in range(1, count):
        peer = lax.rem(me + k, count)
        copies.append(
            remote("ep", peer, norm_ref.at[:, own_cols], land_p.at[k - 1], sems.at[0, k - 1], sems.at[1, k - 1])
        )
        copies.append(
            remote("ep", peer, rows_ref.at[peer], land_a.at[k - 1], sems.at[2, k - 1], sems.at[3, k - 1])
        )
    por_ref[me] = norm_ref[:, own_cols]
    arr_ref[me] = rows_ref[me]
    for k in range(1, count):
        source = lax.rem(me + count - k, count)
        copies[2 * k - 2].wait_recv()
        por_ref[source] = land_p[k - 1]
        copies[2 * k - 1].wait_recv()
        arr_ref[source] = land_a[k - 1]
    for copy in copies:
        copy.wait_send()


def reduce_kernel(
    count, gate_ref, up_ref, moe_ref, hid_ref, sum_ref, land_g, land_u, land_m, hidden, sems
):
    me = greet("tp", count)
    width = sum_ref.shape[1]
    columns = lambda peer: pl.ds(pl.multiple_of(peer * width, width), width)
    dense, moes = [], []
    for k in range(1, count):
        peer = lax.rem(me + k, count)
        for order, (ref, land) in enumerate(((gate_ref, land_g), (up_ref, land_u))):
            dense.append(
                remote("tp", peer, ref.at[peer], land.at[k - 1], sems.at[2 * order, k - 1], sems.at[2 * order + 1, k - 1])
            )
    for k in range(1, count):
        peer = lax.rem(me + k, count)
        moes.append(
            remote("tp", peer, moe_ref.at[:, columns(peer)], land_m.at[k - 1], sems.at[4, k - 1], sems.at[5, k - 1])
        )
    gate_sum = gate_ref[me].astype(F32)
    up_sum = up_ref[me].astype(F32)
    for k in range(1, count):
        dense[2 * k - 2].wait_recv()
        dense[2 * k - 1].wait_recv()
        gate_sum = gate_sum + land_g[k - 1].astype(F32)
        up_sum = up_sum + land_u[k - 1].astype(F32)
    hidden[me] = (jax.nn.silu(gate_sum) * up_sum).astype(BF16)
    finals = []
    for k in range(1, count):
        peer = lax.rem(me + k, count)
        finals.append(
            remote("tp", peer, hidden.at[me], hidden.at[me], sems.at[6, k - 1], sems.at[7, k - 1])
        )
    total = moe_ref[:, columns(me)].astype(F32)
    for k in range(1, count):
        moes[k - 1].wait_recv()
        total = total + land_m[k - 1].astype(F32)
    sum_ref[...] = total.astype(BF16)
    for copy in finals:
        copy.wait_recv()
    hid_ref[...] = hidden[...]
    for copy in dense + moes + finals:
        copy.wait_send()


def gather_kernel(count, dense_ref, moe_ref, out_ref, ret_ref, land_d, land_m, sems):
    me = greet("ep", count)
    copies = []
    for k in range(1, count):
        peer = lax.rem(me + k, count)
        copies.append(
            remote("ep", peer, dense_ref.at[peer], land_d.at[k - 1], sems.at[0, k - 1], sems.at[1, k - 1])
        )
        copies.append(
            remote("ep", peer, moe_ref.at[peer], land_m.at[k - 1], sems.at[2, k - 1], sems.at[3, k - 1])
        )
    total = dense_ref[me].astype(F32)
    ret_ref[me] = moe_ref[me]
    for k in range(1, count):
        copies[2 * k - 2].wait_recv()
        total = total + land_d[k - 1].astype(F32)
        copies[2 * k - 1].wait_recv()
        ret_ref[lax.rem(me + count - k, count)] = land_m[k - 1]
    out_ref[...] = total
    for copy in copies:
        copy.wait_send()


def call_comm(kernel, number, ins, outs, scratch):
    return pl.pallas_call(
        kernel,
        out_shape=[jax.ShapeDtypeStruct(shape, dtype) for shape, dtype in outs],
        in_specs=[VMEM] * len(ins),
        out_specs=[VMEM] * len(outs),
        scratch_shapes=scratch,
        compiler_params=comm_params(number),
        name=f"comm_{number}",
    )(*ins)


def body(
    tokens,
    norm_attn,
    w_query,
    w_key,
    w_value,
    w_forget,
    forget_bias,
    w_output,
    key_cache,
    value_cache,
    gate_cache,
    lengths,
    norm_ffn,
    route_group,
    route_slot,
    route_weight,
    expert_gate,
    expert_up,
    expert_down,
    dense_gate,
    dense_up,
    dense_down,
    mix_vector,
):
    seqs, model = tokens.shape
    ep_count = lax.axis_size("ep")
    tp_count = lax.axis_size("tp")
    tp_position = lax.axis_index("tp")
    width = model // tp_count
    picks = route_slot.shape[1]
    expert_local = expert_gate.shape[0]
    expert_count = expert_local * ep_count
    capacity = seqs // EXPERTS_PER_GROUP
    slots = expert_local * capacity
    dma = pltpu.SemaphoreType.DMA

    flat_ids = (route_group[:, None] * EXPERTS_PER_GROUP + route_slot).reshape(-1)
    matches = flat_ids[:, None] == flat_ids[None, :]
    before = jnp.arange(seqs * picks)[None, :] < jnp.arange(seqs * picks)[:, None]
    earlier = jnp.sum((matches & before).astype(jnp.int32), axis=1)
    slot_ids = (flat_ids * capacity + earlier).reshape(seqs, picks)
    all_slots = jnp.arange(expert_count * capacity, dtype=jnp.int32)
    hits = slot_ids[:, :, None] == all_slots[None, None, :]
    send_table = jnp.any(slot_ids[None, :, :] == all_slots[:, None, None], axis=2).astype(BF16)
    combine_table = jnp.sum(jnp.where(hits, route_weight[:, :, None], 0.0), axis=1)

    head_part = attention(
        tokens, norm_attn, w_query, w_key, w_value, w_forget, forget_bias, w_output,
        key_cache, value_cache, gate_cache, lengths,
    )
    residual, normed_ffn, outgoing = call_comm(
        functools.partial(residual_kernel, tp_count),
        1,
        (head_part, tokens, norm_ffn[None, :], send_table),
        (((seqs, model), F32), ((seqs, model), BF16), ((expert_count * capacity, model), BF16)),
        [pltpu.VMEM((tp_count - 1, seqs, model), BF16), dma((tp_count - 1,)), dma((tp_count - 1,))],
    )
    arrived, portion = call_comm(
        functools.partial(spread_kernel, ep_count, tp_count),
        2,
        (outgoing.reshape(ep_count, slots, model), normed_ffn),
        (((ep_count, slots, model), BF16), ((ep_count, seqs, width), BF16)),
        [
            pltpu.VMEM((ep_count - 1, slots, model), BF16),
            pltpu.VMEM((ep_count - 1, seqs, width), BF16),
            dma((4, ep_count - 1)),
        ],
    )
    portion = portion.reshape(ep_count * seqs, width)
    hidden_local = dense_gate.shape[1]
    tokens_all = ep_count * seqs
    gate_part = jnp.dot(portion, dense_gate, preferred_element_type=F32).astype(BF16)
    up_part = jnp.dot(portion, dense_up, preferred_element_type=F32).astype(BF16)

    arrived = arrived.reshape(ep_count, expert_local, capacity, model)
    gate_act = jnp.einsum("nesd,edf->nesf", arrived, expert_gate, preferred_element_type=F32)
    up_act = jnp.einsum("nesd,edf->nesf", arrived, expert_up, preferred_element_type=F32)
    hidden = (jax.nn.silu(gate_act) * up_act).astype(BF16)
    partial_value = jnp.einsum(
        "nesf,efd->nesd", hidden, expert_down, preferred_element_type=F32
    ).astype(BF16)

    row_part = tokens_all // tp_count
    dense_hidden, summed = call_comm(
        functools.partial(reduce_kernel, tp_count),
        3,
        (
            gate_part.reshape(tp_count, row_part, hidden_local),
            up_part.reshape(tp_count, row_part, hidden_local),
            partial_value.reshape(ep_count * slots, model),
        ),
        (((tp_count, row_part, hidden_local), BF16), ((ep_count * slots, width), BF16)),
        [
            pltpu.VMEM((tp_count - 1, row_part, hidden_local), BF16),
            pltpu.VMEM((tp_count - 1, row_part, hidden_local), BF16),
            pltpu.VMEM((tp_count - 1, ep_count * slots, width), BF16),
            pltpu.VMEM((tp_count, row_part, hidden_local), BF16),
            dma((8, tp_count - 1)),
        ],
    )
    dense_part = jnp.dot(
        dense_hidden.reshape(tokens_all, hidden_local), dense_down, preferred_element_type=F32
    ).astype(BF16)
    dense_out, returned = call_comm(
        functools.partial(gather_kernel, ep_count),
        4,
        (dense_part.reshape(ep_count, seqs, width), summed.reshape(ep_count, slots, width)),
        (((seqs, width), F32), ((ep_count, slots, width), BF16)),
        [
            pltpu.VMEM((ep_count - 1, seqs, width), BF16),
            pltpu.VMEM((ep_count - 1, slots, width), BF16),
            dma((4, ep_count - 1)),
        ],
    )
    returned = returned.reshape(expert_count * capacity, width)
    moe = jnp.dot(combine_table, returned.astype(F32), precision=lax.Precision.HIGHEST)
    mix_gate = jax.nn.sigmoid(
        jnp.dot(normed_ffn.astype(F32), mix_vector, precision=lax.Precision.HIGHEST)
    )
    residual_mine = lax.dynamic_slice_in_dim(residual, tp_position * width, width, 1)
    return (residual_mine + moe + mix_gate[:, None] * dense_out).astype(BF16)


def solution(mesh):
    in_specs = (
        P("ep", None),
        P(),
        P(None, "tp"),
        P(None, "tp"),
        P(None, "tp"),
        P(None, "tp"),
        P("tp"),
        P("tp", None),
        P("ep", None, "tp"),
        P("ep", None, "tp"),
        P("ep", "tp", None),
        P("ep"),
        P(),
        P("ep"),
        P("ep", None),
        P("ep", None),
        P("ep", None, "tp"),
        P("ep", None, "tp"),
        P("ep", "tp", None),
        P("tp", "ep"),
        P("tp", "ep"),
        P("ep", "tp"),
        P(),
    )
    out_specs = P("ep", "tp")
    return jax.shard_map(body, mesh=mesh, in_specs=in_specs, out_specs=out_specs, check_vma=False)
```
